1024 devices in a mesh: ep: 32 (over z, core), tp: 32 (over y, x).
Axes of the slice: x: 4, y: 8, z: 16, core: 2. Of those that a mesh axis runs over, the one named last changes fastest.
Arguments:
- tokens: bfloat16 [512, 4096], P('ep', 'tp'), may hold values from -40 to 40
- norm_gain: bfloat16 [4096], P('tp'), may hold values from 0.099609375 to 1.8984375
- routes: int32 [512, 4], P('ep'), may hold values from 0 to 31, all different within a row; in each aligned block of 16 rows (0 to 15, 16 to 31, ...) at most 4 rows name the same one
- route_weights: float32 [512, 4], P('ep'), may hold values from 0.05 to 1
- w_gate: bfloat16 [32, 4096, 4096], P('ep', None, 'tp'), may hold values from -0.25 to 0.25
- w_up: bfloat16 [32, 4096, 4096], P('ep', None, 'tp'), may hold values from -0.25 to 0.25
- w_down: bfloat16 [32, 4096, 4096], P('ep', 'tp'), may hold values from -0.0234375 to 0.0234375
Outputs:
- mixed: bfloat16 [512, 4096], P('ep', 'tp')
The draws below stay inside these ranges and needn't reach their ends.
Inputs may be any that keep to these rules, and one draw needn't show every extreme that they name: `routes`: within the 16 rows of one device, each token names 4 different experts, and no expert is named by more than 4 rows; some expert reaches 4.
All inputs are finite; a program needn't handle non-finite values.
Results may differ from the reference program's by a relative error of at most 0.018.
Values may be sent and summed in bfloat16 or wider, within the bound.
A program may use at most 64 MiB of HBM per device.

```python
import math
import jax
import jax.numpy as jnp
import numpy as np
from jax import lax

D = 4096
FF = 4096
TOPK = 4
TOK_DEV = 16
EXPERTS = 32
CAP = 4
TOKENS = 512
N_TP = 32


def draw_tokens(key, part):
    first, second, third = jax.random.split(key, 3)
    blocks = max(D // 128, 1)
    width = D // blocks
    column_scale = jnp.exp(jax.random.uniform(second, (blocks,), jnp.float32, -1.1, 1.1))
    column_scale = jnp.repeat(column_scale, width)
    values = jax.random.normal(first, (TOKENS, D), jnp.float32) * column_scale[None, :]
    return jnp.clip(values, -40.0, 40.0).astype(jnp.bfloat16)


def level_of(stream_key, extent, cuts, smallest, top_value):
    level, own = 1.0, jax.random.fold_in(stream_key, 6)
    for axis_at, shards_of in cuts:
        heights = jnp.exp(jax.random.uniform(jax.random.fold_in(own, axis_at), (shards_of,), jnp.float32, smallest / len(cuts), top_value / len(cuts)))
        level = level * jnp.repeat(heights, extent[axis_at] // shards_of).reshape([-1 if axis == axis_at else 1 for axis in range(len(extent))])
    return level


def assign_block(rng, own, number, rows, number_of, top, bound, lean):
    sequence = jax.random.permutation(rng, number_of)
    heavy_load, usual = shares(number_of, rows * top, bound, lean, True), shares(number_of, rows * top, bound, lean, False)
    places = jnp.arange(number_of)

    def named(tallies, turn):
        used = int((tallies > 0).sum())
        fixed = max(1, used // 4)
        moved = fixed + (places - fixed + turn * (used - fixed)) % max(1, number_of - fixed)
        return jnp.zeros((number_of,), jnp.int32).at[sequence[jnp.where(places < fixed, places, moved)]].set(jnp.asarray(tallies, jnp.int32))

    tallies = jnp.where(number % 4 == 0, named(heavy_load, number // 4), named(usual, number - number // 4 - 1))
    mixed = jax.random.permutation(jax.random.fold_in(own, 3), number_of)
    giver, sink = mixed[0:number_of // 2 * 2:2], mixed[1:number_of // 2 * 2:2]
    slack = jnp.minimum(tallies[giver] - 1, bound - tallies[sink]) // 2
    slack = jnp.where((giver == sequence[0]) | (sink == sequence[0]) | (tallies[sink] == 0), 0, jnp.maximum(slack, 0))
    moved = jax.random.randint(jax.random.fold_in(own, 4), (number_of // 2,), 0, 1 << 20) % (slack + 1)
    tallies = tallies.at[giver].add(-moved).at[sink].add(moved)
    labels = jnp.searchsorted(jnp.cumsum(tallies), jnp.arange(rows * top), side="right").astype(jnp.int32)
    table = labels.reshape(top, rows).T
    table = table[jax.random.permutation(jax.random.fold_in(own, 1), rows)]
    turn = jax.random.randint(jax.random.fold_in(own, 2), (rows, 1), 0, top)
    return jnp.take_along_axis(table, (jnp.arange(top)[None, :] + turn) % top, axis=1)


def shares(count, total, limit, skew, full):
    portions = [(1 << 20) // math.isqrt(grade ** skew) + 1 for grade in range(1, count + 1)]
    largest = limit if full else min(limit, max(-(-total // count), total * portions[0] // sum(portions)))
    least = 1 if total - largest >= count - 1 else 0
    holding, rest = [largest] + [least] * (count - 1), total - largest - least * (count - 1)
    while rest > 0:
        free = [i for i in range(1, count) if holding[i] < largest] or [i for i in range(1, count) if holding[i] < limit]
        mass, remaining = sum([portions[i] for i in free]), rest
        for i in free:
            addition = min(limit - holding[i], max(1, remaining * portions[i] // mass), rest)
            holding[i] = holding[i] + addition
            rest = rest - addition
    return np.array(holding)


def scatter_about(own_key, extent, deviation, reach, cuts=(), held_as=jnp.bfloat16):
    array = jax.random.normal(own_key, extent, jnp.float32) * deviation
    if len(cuts) > 0:
        array = level_of(own_key, extent, cuts, -0.22, 0.18) * array
    return jnp.clip(array, min=-reach, max=reach).astype(held_as)


def setup_inputs(seed: int = 0) -> dict:
    arg_keys = jax.random.split(jax.random.key(seed), 8)
    tokens = draw_tokens(jax.random.fold_in(arg_keys[7], 71), 0)
    norm_gain = jnp.clip(1.0 + 0.18 * jax.random.normal(arg_keys[1], (D,), jnp.float32), 0.099609375, 1.8984375).astype(jnp.bfloat16)
    routes_keys = jax.random.split(jax.random.fold_in(arg_keys[2], 1), TOKENS // TOK_DEV)
    routes_turns = jax.random.permutation(jax.random.fold_in(arg_keys[2], 3), TOKENS // TOK_DEV)
    routes = jax.vmap(lambda own, number: assign_block(jax.random.fold_in(arg_keys[2], 2), own, number, TOK_DEV, EXPERTS, TOPK, CAP, 2))(routes_keys, routes_turns).reshape((TOKENS, TOPK))
    route_weights = jnp.clip(0.05 + 0.95 * jax.random.uniform(arg_keys[3], (TOKENS, TOPK), jnp.float32) ** level_of(arg_keys[3], (TOKENS, TOPK), ((0, 32),), -0.2, 0.2), 0.05, 1.0)
    w_gate = scatter_about(arg_keys[4], (EXPERTS, D, FF), (D // 9) ** -0.5, 0.25, ((0, 32), (2, 32)))
    w_up = scatter_about(arg_keys[5], (EXPERTS, D, FF), (D // 9) ** -0.5, 0.25, ((0, 32), (2, 32)))
    w_down = scatter_about(arg_keys[6], (EXPERTS, FF, D), (16 * FF) ** -0.5, 0.0234375, ((0, 32), (1, 32)))
    return dict(tokens=tokens, norm_gain=norm_gain, routes=routes, route_weights=route_weights, w_gate=w_gate, w_up=w_up, w_down=w_down)


def reference(tokens, norm_gain, routes, route_weights, w_gate, w_up, w_down):
    values = tokens.astype(jnp.float32)
    scale = lax.rsqrt(lax.optimization_barrier(jnp.mean(values * values, axis=1, keepdims=True)) + 1e-05)
    normed = (values * scale * norm_gain.astype(jnp.float32)[None, :]).astype(jnp.bfloat16)
    blocks = N_TP
    rows = tokens.shape[0]

    def one_expert(carry, expert):
        gate_pre = jnp.dot(normed, w_gate[expert], preferred_element_type=jnp.float32)
        up_pre = jnp.dot(normed, w_up[expert], preferred_element_type=jnp.float32)
        gated = jnp.minimum(gate_pre, 7.0)
        upper = jnp.clip(up_pre, -7.0, 7.0)
        hidden = ((upper + 1.0) * gated * jax.nn.sigmoid(1.702 * gated)).astype(jnp.bfloat16)
        width = hidden.shape[1] // blocks
        hidden_blocks = hidden.reshape(rows, blocks, width).astype(jnp.float32)
        down_blocks = w_down[expert].reshape(blocks, width, -1).astype(jnp.float32)
        parts = jnp.einsum('tbf,bfd->btd', hidden_blocks, down_blocks).astype(jnp.bfloat16)
        parts = lax.optimization_barrier(parts).astype(jnp.float32)
        result = lax.optimization_barrier(jnp.sum(parts, axis=0)).astype(jnp.bfloat16)
        result = lax.optimization_barrier(result).astype(jnp.float32)
        weight = lax.optimization_barrier(jnp.sum(jnp.where(routes == expert, route_weights, 0.0), axis=1))
        return (carry + weight[:, None] * result, None)
    start = jnp.zeros(tokens.shape, jnp.float32)
    total, _ = lax.scan(one_expert, start, jnp.arange(EXPERTS, dtype=jnp.int32))
    return total.astype(jnp.bfloat16)
```

```python
import functools

import jax
import jax.numpy as jnp
from jax import lax
from jax.experimental import pallas as pl
from jax.experimental.pallas import tpu as pltpu
from jax.sharding import PartitionSpec as P

MESH = pl.DeviceIdType.MESH
BF16 = jnp.bfloat16
F32 = jnp.float32
W = 128
CAP = 4
EPS = 1e-05


def by_distance(n):
    return sorted(range(n), key=lambda j: (min(j, n - j), j))


class Plan:
    def __init__(self, nz, ny, nx):
        self.nz, self.ny, self.nx = nz, ny, nx
        self.experts = 2 * nz
        self.tp = ny * nx
        self.d = self.tp * W
        ring = by_distance(nz)
        self.chunks = [ring[: nz // 2], ring[nz // 2 :]]
        self.pos = {j: at for at, j in enumerate(ring)}
        self.rows = (nz // 2) * 2 * CAP
        self.near = by_distance(ny)
        self.far = self.near[::-1]


def kernel(
    plan,
    tok,
    gain,
    routes,
    rw,
    wg,
    wu,
    wd,
    out,
    wgu_v,
    wd_v,
    ob,
    lb,
    G,
    GA,
    PB,
    XR,
    XM,
    SM,
    Q,
    YL,
    RB,
    RI,
    s_w,
    s_disp,
    r_disp,
    s_gy,
    r_gy,
    s_gx,
    r_gx,
    s_gr,
    r_gr,
    s_xr,
    r_xr,
    s_xm,
    r_xm,
    s_yl,
    r_yl,
    s_ret,
    r_ret,
):
    nz, ny, nx, rows = plan.nz, plan.ny, plan.nx, plan.rows
    ep = lax.axis_index("ep")
    tp = lax.axis_index("tp")
    z, c = ep // 2, ep % 2
    y, x = tp // nx, tp % nx
    right, left, across = (x + 1) % nx, (x + nx - 1) % nx, (x + 2) % nx

    def at_z(j):
        return (z + j) % nz

    def at_y(dy):
        return (y + dy) % ny

    def id_z(j, core):
        return (at_z(j) * 2 + core, tp)

    def id_y(dy):
        return (ep, at_y(dy) * nx + x)

    def id_x(xx):
        return (ep, y * nx + xx)

    peers = [id_z(j, core) for j in range(1, nz) for core in (0, 1)]
    peers += [id_z(0, 1 - c)]
    peers += [id_y(dy) for dy in range(1, ny)]
    peers += [id_x(right), id_x(left)]
    barrier = pltpu.get_barrier_semaphore()
    for peer in peers:
        pl.semaphore_signal(barrier, inc=1, device_id=peer, device_id_type=MESH)

    def weight_copies():
        copies = []
        for yy in range(ny):
            for xx in range(nx):
                block = yy * nx + xx
                for half, src in enumerate((wg, wu)):
                    copies.append(
                        pltpu.make_async_copy(
                            src.at[block],
                            wgu_v.at[xx, pl.ds(yy * W, W), pl.ds(half * W, W)],
                            s_w.at[half, block],
                        )
                    )
        copies.append(pltpu.make_async_copy(wd, wd_v, s_w.at[2, 0]))
        return copies

    weights = weight_copies()
    for copy in weights:
        copy.start()

    tokens = tok.shape[0]
    lanes = plan.experts * CAP
    slot_id = lax.broadcasted_iota(jnp.int32, (tokens, lanes), 1)
    expert_of = slot_id // CAP
    named = jnp.zeros((tokens, lanes), F32)
    weight = jnp.zeros((tokens, lanes), F32)
    for k in range(routes.shape[1]):
        same = routes[:, k : k + 1] == expert_of
        named = jnp.where(same, 1.0, named)
        weight = jnp.where(same, rw[:, k : k + 1], weight)
    lower = (
        lax.broadcasted_iota(jnp.int32, (tokens, tokens), 0)
        > lax.broadcasted_iota(jnp.int32, (tokens, tokens), 1)
    ).astype(F32)
    earlier = jnp.dot(lower, named, preferred_element_type=F32)
    pick = jnp.where(earlier == (slot_id % CAP).astype(F32), named, 0.0)
    combine = weight * pick
    outbound = lax.dot_general(
        pick.astype(BF16),
        tok[...],
        (((0,), (0,)), ((), ())),
        preferred_element_type=F32,
    )
    ob[...] = outbound.reshape(plan.experts, CAP, W).astype(BF16)
    GA[x, y] = jnp.broadcast_to(gain[...], (8, W))
    lb[c] = ob[ep]

    pending = []

    def remote(src, dst, send, recv, device):
        copy = pltpu.make_async_remote_copy(
            src_ref=src,
            dst_ref=dst,
            send_sem=send,
            recv_sem=recv,
            device_id=device,
            device_id_type=MESH,
        )
        copy.start()
        pending.append(copy)
        return copy

    def arrive(ref, sem):
        pltpu.make_async_copy(ref, ref, sem).wait()

    pl.semaphore_wait(barrier, len(peers))

    for j in by_distance(nz)[::-1]:
        landing = plan.pos[(-j) % nz] * 2 + c
        for core in (0, 1) if j else (1 - c,):
            target = at_z(j) * 2 + core
            index = 2 * plan.pos[(-j) % nz] + (core if j else 0)
            remote(
                ob.at[target],
                lb.at[landing],
                s_disp.at[index],
                r_disp.at[landing],
                (target, tp),
            )

    def gather_y(buf, n):
        for dy in plan.far[:-1]:
            remote(buf.at[x, y], buf.at[x, y], s_gy.at[n, dy], r_gy.at[n, (-dy) % ny], id_y(dy))

    def gather_x(buf, n):
        for at, dy in enumerate(plan.near):
            here = buf.at[x, at_y(dy)]
            if dy:
                arrive(here, r_gy.at[n, dy])
            remote(here, here, s_gx.at[n, 0, dy], r_gx.at[n, 0, dy], id_x(right))
            remote(here, here, s_gx.at[n, 1, dy], r_gx.at[n, 1, dy], id_x(left))

    def gather_relay(buf, n):
        for at, dy in enumerate(plan.near):
            way = at % 2
            source, target = (left, right) if way == 0 else (right, left)
            here = buf.at[source, at_y(dy)]
            arrive(here, r_gx.at[n, way, dy])
            remote(here, here, s_gr.at[n, dy], r_gr.at[n, dy], id_x(target))

    def gather_rest(buf, n, which):
        for at, dy in enumerate(plan.near):
            if which == "sides":
                way = 1 - at % 2
                source = left if way == 0 else right
                arrive(buf.at[source, at_y(dy)], r_gx.at[n, way, dy])
            else:
                arrive(buf.at[across, at_y(dy)], r_gr.at[n, dy])

    def chunk_in(k):
        for at in range(len(plan.chunks[k])):
            j = plan.chunks[k][at]
            base = plan.pos[j] * 2
            if j:
                for core in (0, 1):
                    arrive(lb.at[base + core], r_disp.at[base + core])
            else:
                arrive(lb.at[base + 1 - c], r_disp.at[base + 1 - c])
        groups = rows // CAP
        G[k, x, y] = lb[k * groups : (k + 1) * groups].reshape(rows, W)

    def part(k, xx):
        pieces, square = [], jnp.zeros((rows, W), F32)
        for yy in range(ny):
            piece = G[k, xx, yy]
            wide = piece.astype(F32)
            square += wide * wide
            pieces.append(piece * GA[xx, yy][0:1])
        lhs = jnp.concatenate(pieces, axis=1)
        return jnp.dot(lhs, wgu_v[xx], preferred_element_type=F32), square

    def up(k):
        total, square = part(k, x)
        gather_rest(G.at[k], k, "sides")
        for xx in (right, left):
            more, sq = part(k, xx)
            total, square = total + more, square + sq
        gather_rest(G.at[k], k, "across")
        more, sq = part(k, across)
        total, square = total + more, square + sq
        scale = lax.rsqrt(jnp.sum(square, axis=1, keepdims=True) / plan.d + EPS)
        total = total * scale
        gated = jnp.minimum(total[:, :W], 7.0)
        upper = jnp.clip(total[:, W:], -7.0, 7.0)
        return ((upper + 1.0) * gated * jax.nn.sigmoid(1.702 * gated)).astype(BF16)

    def down(k, hidden):
        for yy in range(ny):
            part_out = jnp.dot(
                hidden, wd_v[:, yy * nx * W : (yy + 1) * nx * W], preferred_element_type=F32
            ).astype(BF16)
            for xx in range(nx):
                PB[k, xx, yy] = part_out[:, xx * W : (xx + 1) * W]

    def sum_send(k):
        for at, dy in enumerate(plan.far):
            way = at % 2
            target, other = (right, left) if way == 0 else (left, right)
            remote(PB.at[k, across, at_y(dy)], XR.at[k, dy], s_xr.at[k, dy], r_xr.at[k, dy], id_x(target))
        for at, dy in enumerate(plan.far):
            way = at % 2
            other = left if way == 0 else right
            remote(
                PB.at[k, other, at_y(dy)],
                XM.at[k, 1 - way, dy],
                s_xm.at[k, 1 - way, dy],
                r_xm.at[k, 1 - way, dy],
                id_x(other),
            )

    def sum_relay(k):
        for at, dy in enumerate(plan.far):
            way = at % 2
            target = right if way == 0 else left
            arrive(XR.at[k, dy], r_xr.at[k, dy])
            both = XR[k, dy].astype(F32) + PB[k, target, at_y(dy)].astype(F32)
            SM[k, dy] = both.astype(BF16)
            remote(
                SM.at[k, dy],
                XM.at[k, way, dy],
                s_xm.at[k, way, dy],
                r_xm.at[k, way, dy],
                id_x(target),
            )

    def sum_y(k):
        for dy in plan.far:
            arrive(XM.at[k, 0, dy], r_xm.at[k, 0, dy])
            arrive(XM.at[k, 1, dy], r_xm.at[k, 1, dy])
            total = (
                PB[k, x, at_y(dy)].astype(F32)
                + XM[k, 0, dy].astype(F32)
                + XM[k, 1, dy].astype(F32)
            )
            if dy == 0:
                return total
            Q[k, dy] = total.astype(BF16)
            remote(
                Q.at[k, dy],
                YL.at[k, (-dy) % ny],
                s_yl.at[k, dy],
                r_yl.at[k, (-dy) % ny],
                id_y(dy),
            )

    def sum_end(k, total):
        for dy in plan.near[1:]:
            arrive(YL.at[k, dy], r_yl.at[k, dy])
            total += YL[k, dy].astype(F32)
        groups = rows // CAP
        RB[k * groups : (k + 1) * groups] = total.reshape(groups, CAP, W).astype(BF16)
        for j in plan.chunks[k][::-1]:
            base = plan.pos[j] * 2
            if j == 0:
                RI[ep] = RB[base + c]
            for core in (0, 1) if j else (1 - c,):
                target = at_z(j) * 2 + core
                index = base + (core if j else 0)
                remote(RB.at[base + core], RI.at[ep], s_ret.at[index], r_ret.at[ep], (target, tp))

    gather_y(GA, 2)
    chunk_in(0)
    gather_y(G.at[0], 0)
    gather_x(GA, 2)
    gather_x(G.at[0], 0)
    gather_relay(GA, 2)
    chunk_in(1)
    gather_y(G.at[1], 1)
    gather_relay(G.at[0], 0)
    gather_x(G.at[1], 1)
    gather_rest(GA, 2, "sides")
    gather_rest(GA, 2, "across")
    for copy in weights:
        copy.wait()
    hidden = up(0)
    gather_relay(G.at[1], 1)
    down(0, hidden)
    sum_send(0)
    hidden = up(1)
    down(1, hidden)
    sum_send(1)
    sum_relay(0)
    sum_relay(1)
    first = sum_y(0)
    second = sum_y(1)
    sum_end(1, second)
    sum_end(0, first)

    for j in range(nz):
        for core in (0, 1) if j else (1 - c,):
            expert = at_z(j) * 2 + core
            arrive(RI.at[expert], r_ret.at[expert])
    returned = RI[...].reshape(lanes, W).astype(F32)
    out[...] = jnp.dot(
        combine, returned, preferred_element_type=F32, precision=lax.Precision.HIGHEST
    ).astype(BF16)
    for copy in pending:
        copy.wait_send()


def run(plan, tokens, norm_gain, routes, route_weights, w_gate, w_up, w_down):
    nz, ny, nx, rows = plan.nz, plan.ny, plan.nx, plan.rows
    groups = 2 * nz
    vmem = pl.BlockSpec(memory_space=pltpu.VMEM)
    hbm = pl.BlockSpec(memory_space=pl.ANY)
    dma = pltpu.SemaphoreType.DMA
    return pl.pallas_call(
        functools.partial(kernel, plan),
        out_shape=jax.ShapeDtypeStruct(tokens.shape, BF16),
        in_specs=[vmem] * 4 + [hbm] * 3,
        out_specs=vmem,
        scratch_shapes=[
            pltpu.VMEM((nx, ny * W, 2 * W), BF16),
            pltpu.VMEM((W, plan.d), BF16),
            pltpu.VMEM((groups, CAP, W), BF16),
            pltpu.VMEM((groups, CAP, W), BF16),
            pltpu.VMEM((2, nx, ny, rows, W), BF16),
            pltpu.VMEM((nx, ny, 8, W), BF16),
            pltpu.VMEM((2, nx, ny, rows, W), BF16),
            pltpu.VMEM((2, ny, rows, W), BF16),
            pltpu.VMEM((2, 2, ny, rows, W), BF16),
            pltpu.VMEM((2, ny, rows, W), BF16),
            pltpu.VMEM((2, ny, rows, W), BF16),
            pltpu.VMEM((2, ny, rows, W), BF16),
            pltpu.VMEM((groups, CAP, W), BF16),
            pltpu.VMEM((groups, CAP, W), BF16),
            dma((3, ny * nx)),
            dma((groups,)),
            dma((groups,)),
            dma((3, ny)),
            dma((3, ny)),
            dma((3, 2, ny)),
            dma((3, 2, ny)),
            dma((3, ny)),
            dma((3, ny)),
            dma((2, ny)),
            dma((2, ny)),
            dma((2, 2, ny)),
            dma((2, 2, ny)),
            dma((2, ny)),
            dma((2, ny)),
            dma((groups,)),
            dma((groups,)),
        ],
        compiler_params=pltpu.CompilerParams(collective_id=0, has_side_effects=True),
        name="moe",
    )(
        tokens,
        norm_gain.reshape(1, W),
        routes,
        route_weights,
        w_gate.reshape(ny * nx, W, W),
        w_up.reshape(ny * nx, W, W),
        w_down.reshape(W, plan.d),
    )


def build(mesh, nz, ny, nx):
    placed = (
        P("ep", "tp"),
        P("tp"),
        P("ep", None),
        P("ep", None),
        P("ep", None, "tp"),
        P("ep", None, "tp"),
        P("ep", "tp", None),
    )
    return jax.shard_map(
        functools.partial(run, Plan(nz, ny, nx)),
        mesh=mesh,
        in_specs=placed,
        out_specs=P("ep", "tp"),
        check_vma=False,
    )


def solution(mesh):
    nx = 4
    return build(mesh, mesh.shape["ep"] // 2, mesh.shape["tp"] // nx, nx)
```

```python
import functools

import jax
import jax.numpy as jnp
from jax import lax
from jax.experimental import pallas as pl
from jax.experimental.pallas import tpu as pltpu
from jax.sharding import PartitionSpec as P

MESH = pl.DeviceIdType.MESH
BF16 = jnp.bfloat16
F32 = jnp.float32
W = 128
CAP = 4
EPS = 1e-05


def by_distance(n):
    return sorted(range(n), key=lambda j: (min(j, n - j), j))


class Plan:
    def __init__(self, nz, ny, nx):
        self.nz, self.ny, self.nx = nz, ny, nx
        self.experts = 2 * nz
        self.tp = ny * nx
        self.d = self.tp * W
        ring = by_distance(nz)
        self.chunks = [ring[nz // 2 :], ring[: nz // 2]]
        self.pos = {j: at for at, j in enumerate(self.chunks[0] + self.chunks[1])}
        self.rows = (nz // 2) * 2 * CAP
        self.near = by_distance(ny)
        self.far = self.near[::-1]


def kernel(
    plan,
    tok,
    gain,
    routes,
    rw,
    wg,
    wu,
    wd,
    out,
    wgu_v,
    wd_v,
    ob,
    lb,
    G,
    GA,
    PB,
    XM,
    Q,
    YL,
    RB,
    RI,
    lb2,
    YL2,
    RB2,
    RI2,
    both,
    tok_v,
    gain_v,
    routes_v,
    rw_v,
    s_in,
    s_w,
    s_z,
    s_p,
    r_z,
    r_ga,
    r_gy,
    r_gx,
    r_xm,
    r_yl,
):
    nz, ny, nx, rows = plan.nz, plan.ny, plan.nx, plan.rows
    ep = lax.axis_index("ep")
    tp = lax.axis_index("tp")
    z, c = ep // 2, ep % 2
    y, x = tp // nx, tp % nx

    def at_z(j):
        return (z + j) % nz

    def at_y(dy):
        return (y + dy) % ny

    def id_z(j, core):
        return (at_z(j) * 2 + core, tp)

    def id_y(dy):
        return (ep, at_y(dy) * nx + x)

    def at_x(dx):
        return (x + dx) % nx

    def id_x(dx):
        return (ep, y * nx + at_x(dx))

    sides = [2, 1, 3]
    sides_of = (sides, [1, 3])
    half = [j for j in range(nz) if j in plan.chunks[1] or (-j) % nz in plan.chunks[1]]
    peers = [id_z(j, core) for j in range(1, nz) for core in (0, 1)]
    peers += [id_z(0, 1 - c)]
    peers += [id_y(dy) for dy in range(1, ny)]
    peers += [id_x(dx) for dx in sides]
    facing = y * nx + at_x(2)
    peers += [
        (at_z(j) * 2 + core, facing) for j in half for core in ((0, 1) if j else (1 - c,))
    ]
    barrier = pltpu.get_barrier_semaphore()
    for peer in peers:
        pl.semaphore_signal(barrier, inc=1, device_id=peer, device_id_type=MESH)

    small = [
        pltpu.make_async_copy(src, dst, s_in.at[at])
        for at, (src, dst) in enumerate(
            ((routes, routes_v), (tok, tok_v), (rw, rw_v), (gain, gain_v))
        )
    ]
    for copy in small:
        copy.start()
    for yy in range(ny):
        for xx in range(nx):
            for half, src in enumerate((wg, wu)):
                pltpu.make_async_copy(
                    src.at[yy * nx + xx],
                    wgu_v.at[xx, pl.ds(yy * W, W), pl.ds(half * W, W)],
                    s_w.at[0],
                ).start()
    pltpu.make_async_copy(wd, wd_v, s_w.at[1]).start()
    for copy in small:
        copy.wait()

    tokens = tok.shape[0]
    slots = plan.experts * CAP
    slot_id = lax.broadcasted_iota(jnp.int32, (slots, tokens), 0)
    expert_of = slot_id // CAP
    named = jnp.zeros((slots, tokens), F32)
    weight = jnp.zeros((slots, tokens), F32)
    for k in range(routes.shape[0]):
        same = routes_v[k : k + 1, :] == expert_of
        named = jnp.where(same, 1.0, named)
        weight = jnp.where(same, rw_v[k : k + 1, :], weight)
    before = (
        lax.broadcasted_iota(jnp.int32, (tokens, tokens), 0)
        < lax.broadcasted_iota(jnp.int32, (tokens, tokens), 1)
    ).astype(F32)
    earlier = jnp.dot(named, before, preferred_element_type=F32)
    pick = jnp.where(earlier == (slot_id % CAP).astype(F32), named, 0.0)
    combine = weight * pick
    outbound = jnp.dot(pick.astype(BF16), tok_v[...], preferred_element_type=F32)
    ob[...] = outbound.reshape(plan.experts, CAP, W).astype(BF16)
    GA[x, y] = jnp.broadcast_to(gain_v[...], (8, W))
    lb[2 * plan.pos[0] + c] = ob[ep]

    def remote(src, dst, send, recv, device):
        pltpu.make_async_remote_copy(
            src_ref=src,
            dst_ref=dst,
            send_sem=send,
            recv_sem=recv,
            device_id=device,
            device_id_type=MESH,
        ).start()

    def arrive(ref, sem):
        pltpu.make_async_copy(ref, ref, sem).wait()

    pl.semaphore_wait(barrier, len(peers))

    for j in by_distance(nz)[::-1]:
        landing = plan.pos[(-j) % nz] * 2 + c
        k = 0 if (-j) % nz in plan.chunks[0] else 1
        for core in (0, 1) if j else (1 - c,):
            target = at_z(j) * 2 + core
            remote(ob.at[target], lb.at[landing], s_z.at[0], r_z.at[k], (target, tp))

    groups = rows // CAP
    for j in by_distance(nz)[::-1]:
        back = (-j) % nz
        if back in plan.chunks[1]:
            landing = plan.pos[back] * 2 - groups + c
            for core in (0, 1):
                target = at_z(j) * 2 + core
                remote(ob.at[target], lb2.at[landing], s_z.at[2], r_z.at[3], (target, facing))

    def chunk_in(k):
        arrive(lb.at[pl.ds(0, groups - (1 if k else 0))], r_z.at[k])
        G[k, x, y] = lb[k * groups : (k + 1) * groups].reshape(rows, W)

    def facing_in():
        arrive(lb2, r_z.at[3])
        G[1, at_x(2), y] = lb2[...].reshape(rows, W)
        for dy in plan.far[:-1]:
            here = G.at[1, at_x(2), y]
            remote(here, here, s_p.at[5, 0], r_gx.at[1, 2], id_y(dy))

    def gain_y():
        for dy in plan.far[:-1]:
            remote(GA.at[x, y], GA.at[x, y], s_p.at[4, 0], r_ga.at[0], id_y(dy))

    def gain_x():
        arrive(GA.at[0, pl.ds(0, ny - 1)], r_ga.at[0])
        for dx in sides:
            remote(GA.at[x], GA.at[x], s_p.at[4, 1], r_ga.at[1], id_x(dx))

    def gain_in():
        arrive(GA.at[pl.ds(0, nx - 1)], r_ga.at[1])

    def gather_y(k):
        for dy in plan.far[:-1]:
            here = G.at[k, x, y]
            remote(here, here, s_p.at[k, 0], r_gy.at[k, (-dy) % ny], id_y(dy))

    def gather_x(k, at):
        dy = plan.near[at]
        here = G.at[k, x, at_y(dy)]
        if dy:
            arrive(here, r_gy.at[k, dy])
        for dx in sides_of[k]:
            remote(here, here, s_p.at[k, 1], r_gx.at[k, (-dx) % nx], id_x(dx))

    def part(k, xx):
        pieces, square = [], jnp.zeros((rows, W), F32)
        for yy in range(ny):
            piece = G[k, xx, yy]
            wide = piece.astype(F32)
            square += wide * wide
            pieces.append(piece * GA[xx, yy][0:1])
        lhs = jnp.concatenate(pieces, axis=1)
        return jnp.dot(lhs, wgu_v[xx], preferred_element_type=F32), square

    def up(k):
        total, square = part(k, x)
        for dx in sides[::-1]:
            if k == 1 and dx == 2:
                arrive(G.at[k, at_x(dx), pl.ds(0, ny - 1)], r_gx.at[k, dx])
            else:
                arrive(G.at[k, at_x(dx)], r_gx.at[k, dx])
            more, sq = part(k, at_x(dx))
            total, square = total + more, square + sq
        scale = lax.rsqrt(jnp.sum(square, axis=1, keepdims=True) / plan.d + EPS)
        total = total * scale
        gated = jnp.minimum(total[:, :W], 7.0)
        upper = jnp.clip(total[:, W:], -7.0, 7.0)
        return ((upper + 1.0) * gated * jax.nn.sigmoid(1.702 * gated)).astype(BF16)

    def down(k, hidden):
        for yy in range(ny):
            part_out = jnp.dot(
                hidden, wd_v[:, yy * nx * W : (yy + 1) * nx * W], preferred_element_type=F32
            ).astype(BF16)
            for xx in range(nx):
                PB[k, xx, yy] = part_out[:, xx * W : (xx + 1) * W]

    def sum_x(k):
        for dy in plan.far:
            for dx in sides_of[k]:
                remote(
                    PB.at[k, at_x(dx), at_y(dy)],
                    XM.at[k, dy, (-dx) % nx - 1],
                    s_p.at[2 + k, 1],
                    r_xm.at[k, dy],
                    id_x(dx),
                )

    def facing_out():
        for dy in plan.far[:-1]:
            slot = (-dy) % ny - 1
            remote(PB.at[1, at_x(2), at_y(dy)], YL2.at[slot], s_p.at[5, 1], r_yl.at[2], id_y(dy))

    def sum_y(k):
        for dy in plan.far:
            arrive(XM.at[k, dy, pl.ds(0, len(sides_of[k]))], r_xm.at[k, dy])
            total = PB[k, x, at_y(dy)].astype(F32)
            for dx in sides_of[k]:
                total += XM[k, dy, dx - 1].astype(F32)
            if dy:
                Q[k, dy] = total.astype(BF16)
                slot = (-dy) % ny - 1
                remote(Q.at[k, dy], YL.at[k, slot], s_p.at[2 + k, 0], r_yl.at[k], id_y(dy))
        return total

    def sum_end(k, total):
        arrive(YL.at[k], r_yl.at[k])
        for dy in range(1, ny):
            total += YL[k, dy - 1].astype(F32)
        RB[k * groups : (k + 1) * groups] = total.reshape(groups, CAP, W).astype(BF16)

    def facing_end():
        total = PB[1, at_x(2), y].astype(F32)
        arrive(YL2, r_yl.at[2])
        for dy in range(1, ny):
            total += YL2[dy - 1].astype(F32)
        RB2[...] = total.reshape(groups, CAP, W).astype(BF16)
        for j in plan.chunks[1][::-1]:
            base = 2 * plan.pos[j] - groups
            for core in (0, 1):
                remote(
                    RB2.at[base + core],
                    RI2.at[base + c],
                    s_z.at[3],
                    r_z.at[4],
                    (at_z(j) * 2 + core, facing),
                )

    def give_back(k):
        for j in plan.chunks[k][::-1]:
            base = 2 * plan.pos[j]
            if j == 0:
                RI[ep] = RB[base + c]
            for core in (0, 1) if j else (1 - c,):
                remote(RB.at[base + core], RI.at[ep], s_z.at[1], r_z.at[2], id_z(j, core))

    gain_y()
    chunk_in(1)
    gather_y(1)
    gather_x(1, 0)
    chunk_in(0)
    gather_y(0)
    gather_x(0, 0)
    facing_in()
    gain_x()
    for at in range(1, ny):
        gather_x(1, at)
    for at in range(1, ny):
        gather_x(0, at)
    gain_in()
    arrive(wgu_v, s_w.at[0])
    hidden = up(0)
    arrive(wd_v, s_w.at[1])
    down(0, hidden)
    sum_x(0)
    hidden = up(1)
    down(1, hidden)
    sum_x(1)
    facing_out()
    far = sum_y(0)
    near = sum_y(1)
    sum_end(0, far)
    give_back(0)
    facing_end()
    sum_end(1, near)
    give_back(1)
    arrive(RI2, r_z.at[4])
    arrive(RI.at[pl.ds(0, plan.experts - 1)], r_z.at[2])
    both[...] = RI[...].astype(F32)
    for j in plan.chunks[1]:
        base = 2 * plan.pos[j] - groups
        for core in (0, 1):
            expert = at_z(-j) * 2 + core
            both[expert] = both[expert] + RI2[base + core].astype(F32)
    returned = both[...].reshape(slots, W)
    out[...] = lax.dot_general(
        combine,
        returned,
        (((0,), (0,)), ((), ())),
        preferred_element_type=F32,
        precision=lax.Precision.HIGHEST,
    ).astype(BF16)

    for at in range(2):
        arrive(lb.at[pl.ds(0, plan.experts - 1)], s_z.at[at])
    for k in range(2):
        for buf, at in ((G, k), (PB, 2 + k)):
            arrive(buf.at[k, 0, pl.ds(0, ny - 1)], s_p.at[at, 0])
            arrive(buf.at[k, pl.ds(0, len(sides_of[k]))], s_p.at[at, 1])
    for at in range(2):
        arrive(lb2, s_z.at[2 + at])
        arrive(G.at[1, 0, pl.ds(0, ny - 1)], s_p.at[5, at])
    arrive(GA.at[0, pl.ds(0, ny - 1)], s_p.at[4, 0])
    arrive(GA.at[pl.ds(0, nx - 1)], s_p.at[4, 1])


def run(plan, tokens, norm_gain, routes, route_weights, w_gate, w_up, w_down):
    nz, ny, nx, rows = plan.nz, plan.ny, plan.nx, plan.rows
    groups = 2 * nz
    vmem = pl.BlockSpec(memory_space=pltpu.VMEM)
    hbm = pl.BlockSpec(memory_space=pl.ANY)
    dma = pltpu.SemaphoreType.DMA
    return pl.pallas_call(
        functools.partial(kernel, plan),
        out_shape=jax.ShapeDtypeStruct(tokens.shape, BF16),
        in_specs=[hbm] * 7,
        out_specs=vmem,
        scratch_shapes=[
            pltpu.VMEM((nx, ny * W, 2 * W), BF16),
            pltpu.VMEM((W, plan.d), BF16),
            pltpu.VMEM((groups, CAP, W), BF16),
            pltpu.VMEM((groups, CAP, W), BF16),
            pltpu.VMEM((2, nx, ny, rows, W), BF16),
            pltpu.VMEM((nx, ny, 8, W), BF16),
            pltpu.VMEM((2, nx, ny, rows, W), BF16),
            pltpu.VMEM((2, ny, nx - 1, rows, W), BF16),
            pltpu.VMEM((2, ny, rows, W), BF16),
            pltpu.VMEM((2, ny - 1, rows, W), BF16),
            pltpu.VMEM((groups, CAP, W), BF16),
            pltpu.VMEM((groups, CAP, W), BF16),
            pltpu.VMEM((rows // CAP, CAP, W), BF16),
            pltpu.VMEM((ny - 1, rows, W), BF16),
            pltpu.VMEM((rows // CAP, CAP, W), BF16),
            pltpu.VMEM((rows // CAP, CAP, W), BF16),
            pltpu.VMEM((groups, CAP, W), F32),
            pltpu.VMEM(tokens.shape, BF16),
            pltpu.VMEM((1, W), BF16),
            pltpu.VMEM(routes.shape[::-1], jnp.int32),
            pltpu.VMEM(routes.shape[::-1], F32),
            dma((4,)),
            dma((2,)),
            dma((4,)),
            dma((6, 2)),
            dma((5,)),
            dma((2,)),
            dma((2, ny)),
            dma((2, nx)),
            dma((2, ny)),
            dma((3,)),
        ],
        compiler_params=pltpu.CompilerParams(collective_id=0, has_side_effects=True),
        name="moe",
    )(
        tokens,
        norm_gain.reshape(1, W),
        routes.T,
        route_weights.T,
        w_gate.reshape(ny * nx, W, W),
        w_up.reshape(ny * nx, W, W),
        w_down.reshape(W, plan.d),
    )


def build(mesh, nz, ny, nx):
    placed = (
        P("ep", "tp"),
        P("tp"),
        P("ep", None),
        P("ep", None),
        P("ep", None, "tp"),
        P("ep", None, "tp"),
        P("ep", "tp", None),
    )
    return jax.shard_map(
        functools.partial(run, Plan(nz, ny, nx)),
        mesh=mesh,
        in_specs=placed,
        out_specs=P("ep", "tp"),
        check_vma=False,
    )


def solution(mesh):
    nx = 4
    return build(mesh, mesh.shape["ep"] // 2, mesh.shape["tp"] // nx, nx)
```

```python
import functools

import jax
import jax.numpy as jnp
from jax import lax
from jax.experimental import pallas as pl
from jax.experimental.pallas import tpu as pltpu
from jax.sharding import PartitionSpec as P

MESH = pl.DeviceIdType.MESH
BF16 = jnp.bfloat16
F32 = jnp.float32
W = 128
CAP = 4
EPS = 1e-05


def by_distance(n):
    return sorted(range(n), key=lambda j: (min(j, n - j), j))


class Plan:
    def __init__(self, nz, ny, nx):
        self.nz, self.ny, self.nx = nz, ny, nx
        self.experts = 2 * nz
        self.tp = ny * nx
        self.d = self.tp * W
        ring = by_distance(nz)
        self.chunks = [ring[nz // 2 :], ring[: nz // 2]]
        self.pos = {j: at for at, j in enumerate(self.chunks[0] + self.chunks[1])}
        self.rows = (nz // 2) * 2 * CAP
        self.near = by_distance(ny)
        self.far = self.near[::-1]


def kernel(
    plan,
    tok,
    gain,
    routes,
    rw,
    wg,
    wu,
    wd,
    out,
    wgu_v,
    wd_v,
    ob,
    lb,
    G,
    GA,
    PB,
    XM,
    Q,
    YL,
    RB,
    RI,
    lb2,
    YL2,
    RB2,
    RI2,
    tok_v,
    gain_v,
    routes_v,
    rw_v,
    s_in,
    s_w,
    s_z,
    s_p,
    r_z,
    r_ga,
    r_gy,
    r_gx,
    r_xm,
    r_yl,
):
    nz, ny, nx, rows = plan.nz, plan.ny, plan.nx, plan.rows
    ep = lax.axis_index("ep")
    tp = lax.axis_index("tp")
    z, c = ep // 2, ep % 2
    y, x = tp // nx, tp % nx

    def at_z(j):
        return (z + j) % nz

    def at_y(dy):
        return (y + dy) % ny

    def id_z(j, core):
        return (at_z(j) * 2 + core, tp)

    def id_y(dy):
        return (ep, at_y(dy) * nx + x)

    def at_x(dx):
        return (x + dx) % nx

    def id_x(dx):
        return (ep, y * nx + at_x(dx))

    sides = [2, 1, 3]
    sides_of = (sides, [1, 3])
    half = [j for j in range(nz) if j in plan.chunks[1] or (-j) % nz in plan.chunks[1]]
    peers = [id_z(j, core) for j in range(1, nz) for core in (0, 1)]
    peers += [id_z(0, 1 - c)]
    peers += [id_y(dy) for dy in range(1, ny)]
    peers += [id_x(dx) for dx in sides]
    facing = y * nx + at_x(2)
    peers += [
        (at_z(j) * 2 + core, facing) for j in half for core in ((0, 1) if j else (1 - c,))
    ]
    barrier = pltpu.get_barrier_semaphore()
    for peer in peers:
        pl.semaphore_signal(barrier, inc=1, device_id=peer, device_id_type=MESH)

    small = [
        pltpu.make_async_copy(src, dst, s_in.at[at])
        for at, (src, dst) in enumerate(
            ((routes, routes_v), (tok, tok_v), (rw, rw_v), (gain, gain_v))
        )
    ]
    for copy in small:
        copy.start()
    for yy in range(ny):
        for xx in range(nx):
            for half, src in enumerate((wg, wu)):
                pltpu.make_async_copy(
                    src.at[yy * nx + xx],
                    wgu_v.at[xx, pl.ds(yy * W, W), pl.ds(half * W, W)],
                    s_w.at[0],
                ).start()
    pltpu.make_async_copy(wd, wd_v, s_w.at[1]).start()
    for copy in small:
        copy.wait()

    tokens = tok.shape[0]
    slots = plan.experts * CAP
    slot_id = lax.broadcasted_iota(jnp.int32, (slots, tokens), 0)
    expert_of = slot_id // CAP
    named = jnp.zeros((slots, tokens), F32)
    weight = jnp.zeros((slots, tokens), F32)
    for k in range(routes.shape[0]):
        same = routes_v[k : k + 1, :] == expert_of
        named = jnp.where(same, 1.0, named)
        weight = jnp.where(same, rw_v[k : k + 1, :], weight)
    before = (
        lax.broadcasted_iota(jnp.int32, (tokens, tokens), 0)
        < lax.broadcasted_iota(jnp.int32, (tokens, tokens), 1)
    ).astype(F32)
    earlier = jnp.dot(named, before, preferred_element_type=F32)
    pick = jnp.where(earlier == (slot_id % CAP).astype(F32), named, 0.0)
    combine = weight * pick
    outbound = jnp.dot(pick.astype(BF16), tok_v[...], preferred_element_type=F32)
    ob[...] = outbound.reshape(plan.experts, CAP, W).astype(BF16)
    GA[x, y] = jnp.broadcast_to(gain_v[...], (8, W))
    lb[2 * plan.pos[0] + c] = ob[ep]

    def remote(src, dst, send, recv, device):
        pltpu.make_async_remote_copy(
            src_ref=src,
            dst_ref=dst,
            send_sem=send,
            recv_sem=recv,
            device_id=device,
            device_id_type=MESH,
        ).start()

    def arrive(ref, sem):
        pltpu.make_async_copy(ref, ref, sem).wait()

    pl.semaphore_wait(barrier, len(peers))

    for j in by_distance(nz)[::-1]:
        landing = plan.pos[(-j) % nz] * 2 + c
        k = 0 if (-j) % nz in plan.chunks[0] else 1
        for core in (0, 1) if j else (1 - c,):
            target = at_z(j) * 2 + core
            remote(ob.at[target], lb.at[landing], s_z.at[0], r_z.at[k], (target, tp))

    groups = rows // CAP
    for j in by_distance(nz)[::-1]:
        back = (-j) % nz
        if back in plan.chunks[1]:
            landing = plan.pos[back] * 2 - groups + c
            for core in (0, 1):
                target = at_z(j) * 2 + core
                remote(ob.at[target], lb2.at[landing], s_z.at[2], r_z.at[3], (target, facing))

    def chunk_in(k):
        arrive(lb.at[pl.ds(0, groups - (1 if k else 0))], r_z.at[k])
        G[k, x, y] = lb[k * groups : (k + 1) * groups].reshape(rows, W)

    def facing_in():
        arrive(lb2, r_z.at[3])
        G[1, at_x(2), y] = lb2[...].reshape(rows, W)
        for dy in plan.far[:-1]:
            here = G.at[1, at_x(2), y]
            remote(here, here, s_p.at[5, 0], r_gx.at[1, 2], id_y(dy))

    def gain_y():
        for dy in plan.far[:-1]:
            remote(GA.at[x, y], GA.at[x, y], s_p.at[4, 0], r_ga.at[0], id_y(dy))

    def gain_x():
        arrive(GA.at[0, pl.ds(0, ny - 1)], r_ga.at[0])
        for dx in sides:
            remote(GA.at[x], GA.at[x], s_p.at[4, 1], r_ga.at[1], id_x(dx))

    def gain_in():
        arrive(GA.at[pl.ds(0, nx - 1)], r_ga.at[1])

    def gather_y(k):
        for dy in plan.far[:-1]:
            here = G.at[k, x, y]
            remote(here, here, s_p.at[k, 0], r_gy.at[k, (-dy) % ny], id_y(dy))

    def gather_x(k, at):
        dy = plan.near[at]
        here = G.at[k, x, at_y(dy)]
        if dy:
            arrive(here, r_gy.at[k, dy])
        for dx in sides_of[k]:
            remote(here, here, s_p.at[k, 1], r_gx.at[k, (-dx) % nx], id_x(dx))

    def part(k, xx):
        pieces, square = [], jnp.zeros((rows, W), F32)
        for yy in range(ny):
            piece = G[k, xx, yy]
            wide = piece.astype(F32)
            square += wide * wide
            pieces.append(piece * GA[xx, yy][0:1])
        lhs = jnp.concatenate(pieces, axis=1)
        return jnp.dot(lhs, wgu_v[xx], preferred_element_type=F32), square

    def up(k):
        total, square = part(k, x)
        for dx in sides[::-1]:
            if k == 1 and dx == 2:
                arrive(G.at[k, at_x(dx), pl.ds(0, ny - 1)], r_gx.at[k, dx])
            else:
                arrive(G.at[k, at_x(dx)], r_gx.at[k, dx])
            more, sq = part(k, at_x(dx))
            total, square = total + more, square + sq
        scale = lax.rsqrt(jnp.sum(square, axis=1, keepdims=True) / plan.d + EPS)
        total = total * scale
        gated = jnp.minimum(total[:, :W], 7.0)
        upper = jnp.clip(total[:, W:], -7.0, 7.0)
        return ((upper + 1.0) * gated * jax.nn.sigmoid(1.702 * gated)).astype(BF16)

    def down(k, hidden, send):
        for dy in plan.far:
            yy = at_y(dy)
            columns = pl.ds(pl.multiple_of(yy * (nx * W), nx * W), nx * W)
            part_out = jnp.dot(hidden, wd_v[:, columns], preferred_element_type=F32).astype(BF16)
            for xx in range(nx):
                PB[k, xx, yy] = part_out[:, xx * W : (xx + 1) * W]
            if send:
                sum_x(k, dy)

    def sum_x(k, dy):
        for dx in (1, 3):
            remote(
                PB.at[k, at_x(dx), at_y(dy)],
                XM.at[k, dy, (-dx) % nx - 1],
                s_p.at[2 + k, 1],
                r_xm.at[k, dy],
                id_x(dx),
            )

    def facing_out(k):
        for dy in plan.far[:-1]:
            slot = (-dy) % ny - 1
            remote(
                PB.at[k, at_x(2), at_y(dy)], YL2.at[k, slot], s_p.at[6, k], r_yl.at[2 + k], id_y(dy)
            )

    def sum_y(k):
        for dy in plan.far:
            arrive(XM.at[k, dy, pl.ds(0, 2)], r_xm.at[k, dy])
            total = PB[k, x, at_y(dy)].astype(F32)
            for dx in (1, 3):
                total += XM[k, dy, dx - 1].astype(F32)
            if dy:
                Q[k, dy] = total.astype(BF16)
                slot = (-dy) % ny - 1
                remote(Q.at[k, dy], YL.at[k, slot], s_p.at[2 + k, 0], r_yl.at[k], id_y(dy))
        return total

    def sum_end(k, total):
        arrive(YL.at[k], r_yl.at[k])
        for dy in range(1, ny):
            total += YL[k, dy - 1].astype(F32)
        RB[k * groups : (k + 1) * groups] = total.reshape(groups, CAP, W).astype(BF16)

    def facing_end(k):
        total = PB[k, at_x(2), y].astype(F32)
        arrive(YL2.at[k], r_yl.at[2 + k])
        for dy in range(1, ny):
            total += YL2[k, dy - 1].astype(F32)
        RB2[k * groups : (k + 1) * groups] = total.reshape(groups, CAP, W).astype(BF16)
        for j in plan.chunks[k][::-1]:
            base = 2 * plan.pos[j]
            for core in (0, 1):
                remote(
                    RB2.at[base + core],
                    RI2.at[ep],
                    s_z.at[3],
                    r_z.at[4],
                    (at_z(j) * 2 + core, facing),
                )

    def give_back(k):
        for j in plan.chunks[k][::-1]:
            base = 2 * plan.pos[j]
            if j == 0:
                RI[ep] = RB[base + c]
            for core in (0, 1) if j else (1 - c,):
                remote(RB.at[base + core], RI.at[ep], s_z.at[1], r_z.at[2], id_z(j, core))

    gain_y()
    chunk_in(1)
    gather_y(1)
    gather_x(1, 0)
    chunk_in(0)
    gather_y(0)
    gather_x(0, 0)
    facing_in()
    gain_x()
    for at in range(1, ny):
        gather_x(1, at)
    for at in range(1, ny):
        gather_x(0, at)
    gain_in()
    arrive(wgu_v, s_w.at[0])
    arrive(wd_v, s_w.at[1])
    down(1, up(1), False)
    facing_out(1)
    down(0, up(0), True)
    facing_out(0)
    for dy in plan.far:
        sum_x(1, dy)
    far = sum_y(0)
    near = sum_y(1)
    facing_end(0)
    facing_end(1)
    sum_end(0, far)
    give_back(0)
    sum_end(1, near)
    give_back(1)
    arrive(RI2, r_z.at[4])
    arrive(RI.at[pl.ds(0, plan.experts - 1)], r_z.at[2])
    returned = (RI[...].astype(F32) + RI2[...].astype(F32)).reshape(slots, W)
    out[...] = lax.dot_general(
        combine,
        returned,
        (((0,), (0,)), ((), ())),
        preferred_element_type=F32,
        precision=lax.Precision.HIGHEST,
    )

    for at in range(2):
        arrive(lb.at[pl.ds(0, plan.experts - 1)], s_z.at[at])
    arrive(lb2, s_z.at[2])
    arrive(lb, s_z.at[3])
    for k in range(2):
        row = pl.ds(0, ny - 1)
        arrive(G.at[k, 0, row], s_p.at[k, 0])
        arrive(G.at[k, pl.ds(0, len(sides_of[k]))], s_p.at[k, 1])
        arrive(PB.at[k, 0, row], s_p.at[2 + k, 0])
        arrive(PB.at[k, pl.ds(0, 2)], s_p.at[2 + k, 1])
        arrive(PB.at[k, 0, row], s_p.at[6, k])
    arrive(G.at[1, 0, pl.ds(0, ny - 1)], s_p.at[5, 0])
    arrive(GA.at[0, pl.ds(0, ny - 1)], s_p.at[4, 0])
    arrive(GA.at[pl.ds(0, nx - 1)], s_p.at[4, 1])


def run(plan, tokens, norm_gain, routes, route_weights, w_gate, w_up, w_down):
    nz, ny, nx, rows = plan.nz, plan.ny, plan.nx, plan.rows
    groups = 2 * nz
    vmem = pl.BlockSpec(memory_space=pltpu.VMEM)
    hbm = pl.BlockSpec(memory_space=pl.ANY)
    dma = pltpu.SemaphoreType.DMA
    return pl.pallas_call(
        functools.partial(kernel, plan),
        out_shape=pltpu.VMEM(tokens.shape, F32),
        in_specs=[hbm] * 7,
        out_specs=vmem,
        scratch_shapes=[
            pltpu.VMEM((nx, ny * W, 2 * W), BF16),
            pltpu.VMEM((W, plan.d), BF16),
            pltpu.VMEM((groups, CAP, W), BF16),
            pltpu.VMEM((groups, CAP, W), BF16),
            pltpu.VMEM((2, nx, ny, rows, W), BF16),
            pltpu.VMEM((nx, ny, 8, W), BF16),
            pltpu.VMEM((2, nx, ny, rows, W), BF16),
            pltpu.VMEM((2, ny, nx - 1, rows, W), BF16),
            pltpu.VMEM((2, ny, rows, W), BF16),
            pltpu.VMEM((2, ny - 1, rows, W), BF16),
            pltpu.VMEM((groups, CAP, W), BF16),
            pltpu.VMEM((groups, CAP, W), BF16),
            pltpu.VMEM((rows // CAP, CAP, W), BF16),
            pltpu.VMEM((2, ny - 1, rows, W), BF16),
            pltpu.VMEM((groups, CAP, W), BF16),
            pltpu.VMEM((groups, CAP, W), BF16),
            pltpu.VMEM(tokens.shape, BF16),
            pltpu.VMEM((1, W), BF16),
            pltpu.VMEM(routes.shape[::-1], jnp.int32),
            pltpu.VMEM(routes.shape[::-1], F32),
            dma((4,)),
            dma((2,)),
            dma((4,)),
            dma((7, 2)),
            dma((5,)),
            dma((2,)),
            dma((2, ny)),
            dma((2, nx)),
            dma((2, ny)),
            dma((4,)),
        ],
        compiler_params=pltpu.CompilerParams(collective_id=0, has_side_effects=True),
        name="moe",
    )(
        tokens,
        norm_gain.reshape(1, W),
        routes.T,
        route_weights.T,
        w_gate.reshape(ny * nx, W, W),
        w_up.reshape(ny * nx, W, W),
        w_down.reshape(W, plan.d),
    ).astype(BF16)


def build(mesh, nz, ny, nx):
    placed = (
        P("ep", "tp"),
        P("tp"),
        P("ep", None),
        P("ep", None),
        P("ep", None, "tp"),
        P("ep", None, "tp"),
        P("ep", "tp", None),
    )
    return jax.shard_map(
        functools.partial(run, Plan(nz, ny, nx)),
        mesh=mesh,
        in_specs=placed,
        out_specs=P("ep", "tp"),
        check_vma=False,
    )


def solution(mesh):
    nx = 4
    return build(mesh, mesh.shape["ep"] // 2, mesh.shape["tp"] // nx, nx)
```

```python
import functools

import jax
import jax.numpy as jnp
from jax import lax
from jax.experimental import pallas as pl
from jax.experimental.pallas import tpu as pltpu
from jax.sharding import PartitionSpec as P

MESH = pl.DeviceIdType.MESH
BF16 = jnp.bfloat16
F32 = jnp.float32
W = 128
CAP = 4
EPS = 1e-05


def by_distance(n):
    return sorted(range(n), key=lambda j: (min(j, n - j), j))


class Plan:
    def __init__(self, nz, ny, nx):
        self.nz, self.ny, self.nx = nz, ny, nx
        self.experts = 2 * nz
        self.tp = ny * nx
        self.d = self.tp * W
        ring = by_distance(nz)
        self.chunks = [ring[nz // 2 :], ring[: nz // 2]]
        self.pos = {j: at for at, j in enumerate(self.chunks[0] + self.chunks[1])}
        self.rows = (nz // 2) * 2 * CAP
        self.near = by_distance(ny)
        self.far = self.near[::-1]


def kernel(
    plan,
    tok,
    gain,
    routes,
    rw,
    wg,
    wu,
    wd,
    out,
    wgu_v,
    wd_v,
    ob,
    lb,
    G,
    GA,
    PB,
    XM,
    Q,
    YL,
    RB,
    RI,
    lb2,
    YL2,
    RB2,
    RI2,
    tok_v,
    gain_v,
    routes_v,
    rw_v,
    s_in,
    s_w,
    s_z,
    s_p,
    r_z,
    r_ga,
    r_gy,
    r_gx,
    r_xm,
    r_yl,
):
    nz, ny, nx, rows = plan.nz, plan.ny, plan.nx, plan.rows
    ep = lax.axis_index("ep")
    tp = lax.axis_index("tp")
    z, c = ep // 2, ep % 2
    y, x = tp // nx, tp % nx

    def at_z(j):
        return (z + j) % nz

    def at_y(dy):
        return (y + dy) % ny

    def id_z(j, core):
        return (at_z(j) * 2 + core, tp)

    def id_y(dy):
        return (ep, at_y(dy) * nx + x)

    def at_x(dx):
        return (x + dx) % nx

    def id_x(dx):
        return (ep, y * nx + at_x(dx))

    sides = [2, 1, 3]
    sides_of = (sides, [1, 3])
    half = [j for j in range(nz) if j in plan.chunks[1] or (-j) % nz in plan.chunks[1]]
    peers = [id_z(j, core) for j in by_distance(nz)[:0:-1] for core in (0, 1)]
    peers += [id_z(0, 1 - c)]
    peers += [id_y(dy) for dy in range(1, ny)]
    peers += [id_x(dx) for dx in sides]
    facing = y * nx + at_x(2)
    peers += [
        (at_z(j) * 2 + core, facing) for j in half for core in ((0, 1) if j else (1 - c,))
    ]
    barrier = pltpu.get_barrier_semaphore()
    for peer in peers:
        pl.semaphore_signal(barrier, inc=1, device_id=peer, device_id_type=MESH)

    small = [
        pltpu.make_async_copy(src, dst, s_in.at[at])
        for at, (src, dst) in enumerate(
            ((routes, routes_v), (tok, tok_v), (rw, rw_v), (gain, gain_v))
        )
    ]
    for copy in small:
        copy.start()
    for copy in small:
        copy.wait()

    tokens = tok.shape[0]
    slots = plan.experts * CAP
    slot_id = lax.broadcasted_iota(jnp.int32, (slots, tokens), 0)
    expert_of = slot_id // CAP
    named = jnp.zeros((slots, tokens), F32)
    weight = jnp.zeros((slots, tokens), F32)
    for k in range(routes.shape[0]):
        same = routes_v[k : k + 1, :] == expert_of
        named = jnp.where(same, 1.0, named)
        weight = jnp.where(same, rw_v[k : k + 1, :], weight)
    before = (
        lax.broadcasted_iota(jnp.int32, (tokens, tokens), 0)
        < lax.broadcasted_iota(jnp.int32, (tokens, tokens), 1)
    ).astype(F32)
    earlier = jnp.dot(named, before, preferred_element_type=F32)
    pick = jnp.where(earlier == (slot_id % CAP).astype(F32), named, 0.0)
    combine = weight * pick
    outbound = jnp.dot(pick.astype(BF16), tok_v[...], preferred_element_type=F32)
    ob[...] = outbound.reshape(plan.experts, CAP, W).astype(BF16)
    GA[x, y] = jnp.broadcast_to(gain_v[...], (8, W))
    lb[2 * plan.pos[0] + c] = ob[ep]

    def remote(src, dst, send, recv, device):
        pltpu.make_async_remote_copy(
            src_ref=src,
            dst_ref=dst,
            send_sem=send,
            recv_sem=recv,
            device_id=device,
            device_id_type=MESH,
        ).start()

    def arrive(ref, sem):
        pltpu.make_async_copy(ref, ref, sem).wait()

    pl.semaphore_wait(barrier, len(peers))

    for j in by_distance(nz)[::-1]:
        landing = plan.pos[(-j) % nz] * 2 + c
        k = 0 if (-j) % nz in plan.chunks[0] else 1
        for core in (0, 1) if j else (1 - c,):
            target = at_z(j) * 2 + core
            remote(ob.at[target], lb.at[landing], s_z.at[0], r_z.at[k], (target, tp))

    groups = rows // CAP
    for j in by_distance(nz)[::-1]:
        back = (-j) % nz
        if back in plan.chunks[1]:
            landing = plan.pos[back] * 2 - groups + c
            for core in (0, 1):
                target = at_z(j) * 2 + core
                remote(ob.at[target], lb2.at[landing], s_z.at[2], r_z.at[3], (target, facing))

    def chunk_in(k):
        arrive(lb.at[pl.ds(0, groups - (1 if k else 0))], r_z.at[k])
        G[k, x, y] = lb[k * groups : (k + 1) * groups].reshape(rows, W)

    def facing_in():
        arrive(lb2, r_z.at[3])
        G[1, at_x(2), y] = lb2[...].reshape(rows, W)
        for dy in plan.far[:-1]:
            here = G.at[1, at_x(2), y]
            remote(here, here, s_p.at[5, 0], r_gx.at[1, 2], id_y(dy))

    def gain_y():
        for dy in plan.far[:-1]:
            remote(GA.at[x, y], GA.at[x, y], s_p.at[4, 0], r_ga.at[0], id_y(dy))

    def gain_x():
        arrive(GA.at[0, pl.ds(0, ny - 1)], r_ga.at[0])
        for dx in sides:
            remote(GA.at[x], GA.at[x], s_p.at[4, 1], r_ga.at[1], id_x(dx))

    def gain_in():
        arrive(GA.at[pl.ds(0, nx - 1)], r_ga.at[1])

    def gather_y(k):
        for dy in plan.far[:-1]:
            here = G.at[k, x, y]
            remote(here, here, s_p.at[k, 0], r_gy.at[k, (-dy) % ny], id_y(dy))

    def gather_x(k, at):
        dy = plan.near[at]
        here = G.at[k, x, at_y(dy)]
        if dy:
            arrive(here, r_gy.at[k, dy])
        for dx in sides_of[k]:
            remote(here, here, s_p.at[k, 1], r_gx.at[k, (-dx) % nx], id_x(dx))

    def part(k, xx):
        pieces, square = [], jnp.zeros((rows, W), F32)
        for yy in range(ny):
            piece = G[k, xx, yy]
            wide = piece.astype(F32)
            square += wide * wide
            pieces.append(piece * GA[xx, yy][0:1])
        lhs = jnp.concatenate(pieces, axis=1)
        return jnp.dot(lhs, wgu_v[xx], preferred_element_type=F32), square

    def up(k):
        total, square = part(k, x)
        for dx in sides[::-1]:
            if k == 1 and dx == 2:
                arrive(G.at[k, at_x(dx), pl.ds(0, ny - 1)], r_gx.at[k, dx])
            else:
                arrive(G.at[k, at_x(dx)], r_gx.at[k, dx])
            more, sq = part(k, at_x(dx))
            total, square = total + more, square + sq
        scale = lax.rsqrt(jnp.sum(square, axis=1, keepdims=True) / plan.d + EPS)
        total = total * scale
        gated = jnp.minimum(total[:, :W], 7.0)
        upper = jnp.clip(total[:, W:], -7.0, 7.0)
        return ((upper + 1.0) * gated * jax.nn.sigmoid(1.702 * gated)).astype(BF16)

    def down(k, hidden, send):
        for dy in plan.far:
            yy = at_y(dy)
            columns = pl.ds(pl.multiple_of(yy * (nx * W), nx * W), nx * W)
            part_out = jnp.dot(hidden, wd_v[:, columns], preferred_element_type=F32).astype(BF16)
            for xx in range(nx):
                PB[k, xx, yy] = part_out[:, xx * W : (xx + 1) * W]
            if send:
                sum_x(k, dy)

    def sum_x(k, dy):
        for dx in (1, 3):
            remote(
                PB.at[k, at_x(dx), at_y(dy)],
                XM.at[k, dy, (-dx) % nx - 1],
                s_p.at[2 + k, 1],
                r_xm.at[k, dy],
                id_x(dx),
            )

    def facing_out(k):
        for dy in plan.far[:-1]:
            slot = (-dy) % ny - 1
            remote(
                PB.at[k, at_x(2), at_y(dy)], YL2.at[k, slot], s_p.at[6, k], r_yl.at[2 + k], id_y(dy)
            )

    def sum_y(k):
        for dy in plan.far:
            arrive(XM.at[k, dy, pl.ds(0, 2)], r_xm.at[k, dy])
            total = PB[k, x, at_y(dy)].astype(F32)
            for dx in (1, 3):
                total += XM[k, dy, dx - 1].astype(F32)
            if dy:
                Q[k, dy] = total.astype(BF16)
                slot = (-dy) % ny - 1
                remote(Q.at[k, dy], YL.at[k, slot], s_p.at[2 + k, 0], r_yl.at[k], id_y(dy))
        return total

    def sum_end(k, total):
        arrive(YL.at[k], r_yl.at[k])
        for dy in range(1, ny):
            total += YL[k, dy - 1].astype(F32)
        RB[k * groups : (k + 1) * groups] = total.reshape(groups, CAP, W).astype(BF16)

    def facing_end(k):
        total = PB[k, at_x(2), y].astype(F32)
        arrive(YL2.at[k], r_yl.at[2 + k])
        for dy in range(1, ny):
            total += YL2[k, dy - 1].astype(F32)
        RB2[k * groups : (k + 1) * groups] = total.reshape(groups, CAP, W).astype(BF16)
        for j in plan.chunks[k][::-1]:
            base = 2 * plan.pos[j]
            for core in (0, 1):
                remote(
                    RB2.at[base + core],
                    RI2.at[ep],
                    s_z.at[3],
                    r_z.at[4],
                    (at_z(j) * 2 + core, facing),
                )

    def give_back(k):
        for j in plan.chunks[k][::-1]:
            base = 2 * plan.pos[j]
            if j == 0:
                RI[ep] = RB[base + c]
            for core in (0, 1) if j else (1 - c,):
                remote(RB.at[base + core], RI.at[ep], s_z.at[1], r_z.at[2], id_z(j, core))

    gain_y()
    for yy in range(ny):
        for xx in range(nx):
            for half, src in enumerate((wg, wu)):
                pltpu.make_async_copy(
                    src.at[yy * nx + xx],
                    wgu_v.at[xx, pl.ds(yy * W, W), pl.ds(half * W, W)],
                    s_w.at[0],
                ).start()
    pltpu.make_async_copy(wd, wd_v, s_w.at[1]).start()
    chunk_in(1)
    gather_y(1)
    gather_x(1, 0)
    chunk_in(0)
    gather_y(0)
    gather_x(0, 0)
    facing_in()
    gain_x()
    for at in range(1, ny):
        gather_x(1, at)
    for at in range(1, ny):
        gather_x(0, at)
    gain_in()
    arrive(wgu_v, s_w.at[0])
    arrive(wd_v, s_w.at[1])
    down(1, up(1), False)
    facing_out(1)
    down(0, up(0), True)
    facing_out(0)
    for dy in plan.far:
        sum_x(1, dy)
    far = sum_y(0)
    near = sum_y(1)
    facing_end(0)
    facing_end(1)
    sum_end(0, far)
    give_back(0)
    sum_end(1, near)
    give_back(1)
    arrive(RI2, r_z.at[4])
    arrive(RI.at[pl.ds(0, plan.experts - 1)], r_z.at[2])
    returned = (RI[...].astype(F32) + RI2[...].astype(F32)).reshape(slots, W)
    out[...] = lax.dot_general(
        combine,
        returned,
        (((0,), (0,)), ((), ())),
        preferred_element_type=F32,
        precision=lax.Precision.HIGHEST,
    )

    for at in range(2):
        arrive(lb.at[pl.ds(0, plan.experts - 1)], s_z.at[at])
    arrive(lb2, s_z.at[2])
    arrive(lb, s_z.at[3])
    for k in range(2):
        row = pl.ds(0, ny - 1)
        arrive(G.at[k, 0, row], s_p.at[k, 0])
        arrive(G.at[k, pl.ds(0, len(sides_of[k]))], s_p.at[k, 1])
        arrive(PB.at[k, 0, row], s_p.at[2 + k, 0])
        arrive(PB.at[k, pl.ds(0, 2)], s_p.at[2 + k, 1])
        arrive(PB.at[k, 0, row], s_p.at[6, k])
    arrive(G.at[1, 0, pl.ds(0, ny - 1)], s_p.at[5, 0])
    arrive(GA.at[0, pl.ds(0, ny - 1)], s_p.at[4, 0])
    arrive(GA.at[pl.ds(0, nx - 1)], s_p.at[4, 1])


def run(plan, tokens, norm_gain, routes, route_weights, w_gate, w_up, w_down):
    nz, ny, nx, rows = plan.nz, plan.ny, plan.nx, plan.rows
    groups = 2 * nz
    vmem = pl.BlockSpec(memory_space=pltpu.VMEM)
    hbm = pl.BlockSpec(memory_space=pl.ANY)
    dma = pltpu.SemaphoreType.DMA
    return pl.pallas_call(
        functools.partial(kernel, plan),
        out_shape=pltpu.VMEM(tokens.shape, F32),
        in_specs=[hbm] * 7,
        out_specs=vmem,
        scratch_shapes=[
            pltpu.VMEM((nx, ny * W, 2 * W), BF16),
            pltpu.VMEM((W, plan.d), BF16),
            pltpu.VMEM((groups, CAP, W), BF16),
            pltpu.VMEM((groups, CAP, W), BF16),
            pltpu.VMEM((2, nx, ny, rows, W), BF16),
            pltpu.VMEM((nx, ny, 8, W), BF16),
            pltpu.VMEM((2, nx, ny, rows, W), BF16),
            pltpu.VMEM((2, ny, nx - 1, rows, W), BF16),
            pltpu.VMEM((2, ny, rows, W), BF16),
            pltpu.VMEM((2, ny - 1, rows, W), BF16),
            pltpu.VMEM((groups, CAP, W), BF16),
            pltpu.VMEM((groups, CAP, W), BF16),
            pltpu.VMEM((rows // CAP, CAP, W), BF16),
            pltpu.VMEM((2, ny - 1, rows, W), BF16),
            pltpu.VMEM((groups, CAP, W), BF16),
            pltpu.VMEM((groups, CAP, W), BF16),
            pltpu.VMEM(tokens.shape, BF16),
            pltpu.VMEM((1, W), BF16),
            pltpu.VMEM(routes.shape[::-1], jnp.int32),
            pltpu.VMEM(routes.shape[::-1], F32),
            dma((4,)),
            dma((2,)),
            dma((4,)),
            dma((7, 2)),
            dma((5,)),
            dma((2,)),
            dma((2, ny)),
            dma((2, nx)),
            dma((2, ny)),
            dma((4,)),
        ],
        compiler_params=pltpu.CompilerParams(collective_id=0, has_side_effects=True),
        name="moe",
    )(
        tokens,
        norm_gain.reshape(1, W),
        routes.T,
        route_weights.T,
        w_gate.reshape(ny * nx, W, W),
        w_up.reshape(ny * nx, W, W),
        w_down.reshape(W, plan.d),
    ).astype(BF16)


def build(mesh, nz, ny, nx):
    placed = (
        P("ep", "tp"),
        P("tp"),
        P("ep", None),
        P("ep", None),
        P("ep", None, "tp"),
        P("ep", None, "tp"),
        P("ep", "tp", None),
    )
    return jax.shard_map(
        functools.partial(run, Plan(nz, ny, nx)),
        mesh=mesh,
        in_specs=placed,
        out_specs=P("ep", "tp"),
        check_vma=False,
    )


def solution(mesh):
    nx = 4
    return build(mesh, mesh.shape["ep"] // 2, mesh.shape["tp"] // nx, nx)
```
